32 devices in a mesh: sp: 16 (over z, y, core), tp: 2 (over x).
Axes of the slice: x: 2, y: 2, z: 4, core: 2. Of those that a mesh axis runs over, the one named last changes fastest.
Arguments:
- tokens: bfloat16 [1536, 2048], P('sp'), may hold values from -2500 to 2500
- query_down: bfloat16 [2048, 512], replicated, may hold values from -0.125 to 0.125
- latent_down: bfloat16 [2048, 512], replicated, may hold values from -0.125 to 0.125
- rope_down: bfloat16 [2048, 64], replicated, may hold values from -0.125 to 0.125
- query_gain: float32 [512], replicated, may hold values from 0.1 to 1.9
- latent_gain: float32 [512], replicated, may hold values from 0.1 to 1.9
- query_up: bfloat16 [512, 512], P(None, 'tp'), may hold values from -0.25 to 0.25
- query_rope: bfloat16 [512, 256], P(None, 'tp'), may hold values from -0.25 to 0.25
- key_up: bfloat16 [512, 512], P(None, 'tp'), may hold values from -0.25 to 0.25
- value_up: bfloat16 [512, 512], P(None, 'tp'), may hold values from -0.25 to 0.25
- out_proj: bfloat16 [512, 2048], replicated, may hold values from -0.25 to 0.25
- out_gain: float32 [2048], replicated, may hold values from 0.1 to 1.9
Outputs:
- mixed: bfloat16 [1536, 2048], P('sp')
The draws below stay inside these ranges and needn't reach their ends.
All inputs are finite; a program needn't handle non-finite values.
Results may differ from the reference program's by a relative error of at most 0.035.
Values may be sent and summed in bfloat16 or wider, within the bound.
A program may use at most 64 MiB of HBM per device.

```python
import math
import jax
import jax.numpy as jnp
from jax import lax

D = 2048
HEADS = 4
NOPE = 128
ROPE = 64
VDIM = 128
QLAT = 512
KVLAT = 512
SEQS = 8
SEQ_SP = 96
LEN = 192
ROWS = 1536


def draw_tokens(key, part):
    noise_key = jax.random.fold_in(key, 11)
    mean_key = jax.random.fold_in(key, 12)
    blocks = ROWS // SEQ_SP
    noise = jnp.clip(jax.random.normal(noise_key, (ROWS, D), jnp.float32), -6.0, 6.0)
    means = 0.7 * jnp.clip(jax.random.normal(mean_key, (blocks, D), jnp.float32), -3.0, 3.0)
    shifted = jnp.repeat(means, SEQ_SP, axis=0, total_repeat_length=ROWS)
    return (noise + shifted).astype(jnp.bfloat16)


def levels(stream_key, dims, shards, least, high):
    level = 1.0
    for axis_at, blocks in shards:
        steps = jax.random.uniform(jax.random.fold_in(jax.random.fold_in(stream_key, 6), axis_at), (blocks,), jnp.float32, least / len(shards), high / len(shards))
        level = level * jnp.repeat(jnp.exp(steps), dims[axis_at] // blocks).reshape((-1,) + (1,) * (len(dims) - 1 - axis_at))
    return level


def bell_draw(stream_key, dims, scale, reach, shards=(), kind=jnp.bfloat16):
    loudness = levels(stream_key, dims, shards, -0.22, 0.18) if shards else 1.0
    entries = jax.random.normal(stream_key, dims, jnp.float32) * scale * loudness
    return jnp.minimum(jnp.maximum(entries, -reach), reach).astype(kind)


def setup_inputs(seed: int = 0) -> dict:
    arg_keys = jax.random.split(jax.random.key(seed), 13)
    tokens = draw_tokens(jax.random.fold_in(arg_keys[12], 71), 0)
    query_down = bell_draw(arg_keys[1], (D, QLAT), D ** -0.5, 0.125)
    latent_down = bell_draw(arg_keys[2], (D, KVLAT), D ** -0.5, 0.125)
    rope_down = bell_draw(arg_keys[3], (D, ROPE), D ** -0.5, 0.125)
    query_gain = jnp.clip(1.0 + 0.18 * jax.random.normal(arg_keys[4], (QLAT,), jnp.float32), 0.1, 1.9)
    latent_gain = jnp.clip(1.0 + 0.18 * jax.random.normal(arg_keys[5], (KVLAT,), jnp.float32), 0.1, 1.9)
    query_up = bell_draw(arg_keys[6], (QLAT, HEADS * NOPE), QLAT ** -0.5, 0.25, ((1, 2),))
    query_rope = bell_draw(arg_keys[7], (QLAT, HEADS * ROPE), QLAT ** -0.5, 0.25, ((1, 2),))
    key_up = bell_draw(arg_keys[8], (KVLAT, HEADS * NOPE), KVLAT ** -0.5, 0.25, ((1, 2),))
    value_up = bell_draw(arg_keys[9], (KVLAT, HEADS * VDIM), KVLAT ** -0.5, 0.25, ((1, 2),))
    out_proj = bell_draw(arg_keys[10], (HEADS * VDIM, D), (HEADS * VDIM) ** -0.5, 0.25)
    out_gain = jnp.clip(1.0 + 0.18 * jax.random.normal(arg_keys[11], (D,), jnp.float32), 0.1, 1.9)
    return dict(tokens=tokens, query_down=query_down, latent_down=latent_down, rope_down=rope_down, query_gain=query_gain, latent_gain=latent_gain, query_up=query_up, query_rope=query_rope, key_up=key_up, value_up=value_up, out_proj=out_proj, out_gain=out_gain)


EPS = 1e-06
THETA = 10000.0

def normalize(rows, gain):
    mean_sq = lax.optimization_barrier(jnp.mean(rows * rows, axis=-1, keepdims=True))
    return rows * lax.rsqrt(mean_sq + EPS) * gain.astype(jnp.float32)

def angles(positions, width):
    half = width // 2
    freq = THETA ** (-jnp.arange(half, dtype=jnp.float32) / half)
    angle = positions[:, None] * freq[None, :]
    return (jnp.cos(angle), jnp.sin(angle))

def rotate(rows, cosine, sine):
    half = rows.shape[-1] // 2
    first = rows[..., :half]
    second = rows[..., half:]
    return jnp.concatenate([first * cosine - second * sine, first * sine + second * cosine], axis=-1)

def reference(tokens, query_down, latent_down, rope_down, query_gain, latent_gain, query_up, query_rope, key_up, value_up, out_proj, out_gain):
    scale = (NOPE + ROPE) ** (-0.5)
    positions = jnp.arange(LEN, dtype=jnp.int32).astype(jnp.float32)
    cosine, sine = angles(positions, ROPE)
    block = math.gcd(LEN, 512)
    starts = jnp.arange(LEN // block, dtype=jnp.int32) * block

    def one_sequence(seq_rows):
        q_latent = normalize(jnp.dot(seq_rows, query_down, preferred_element_type=jnp.float32), query_gain).astype(jnp.bfloat16)
        kv_latent = normalize(jnp.dot(seq_rows, latent_down, preferred_element_type=jnp.float32), latent_gain).astype(jnp.bfloat16)
        rope_key = rotate(jnp.dot(seq_rows, rope_down, preferred_element_type=jnp.float32), cosine, sine).astype(jnp.bfloat16)
        q_nope = jnp.dot(q_latent, query_up, preferred_element_type=jnp.float32).astype(jnp.bfloat16).reshape(LEN, HEADS, NOPE)
        q_rot = rotate(jnp.dot(q_latent, query_rope, preferred_element_type=jnp.float32).reshape(LEN, HEADS, ROPE), cosine[:, None, :], sine[:, None, :]).astype(jnp.bfloat16)
        keys = jnp.dot(kv_latent, key_up, preferred_element_type=jnp.float32).astype(jnp.bfloat16)
        keys = keys.reshape(LEN, HEADS, NOPE).astype(jnp.float32)
        values = jnp.dot(kv_latent, value_up, preferred_element_type=jnp.float32).astype(jnp.bfloat16)
        values = values.reshape(LEN, HEADS, VDIM).astype(jnp.float32)
        rope_wide = rope_key.astype(jnp.float32)

        def one_block(start):
            query_block = lax.dynamic_slice_in_dim(q_nope, start, block, 0).astype(jnp.float32)
            rot_block = lax.dynamic_slice_in_dim(q_rot, start, block, 0).astype(jnp.float32)
            scores = (jnp.einsum('qhd,khd->hqk', query_block, keys) + jnp.einsum('qhr,kr->hqk', rot_block, rope_wide)) * scale
            highest = lax.optimization_barrier(jnp.max(scores, axis=-1, keepdims=True))
            expd = jnp.exp(scores - highest)
            total = lax.optimization_barrier(jnp.sum(expd, axis=-1))
            probs = lax.optimization_barrier(expd.astype(jnp.bfloat16)).astype(jnp.float32)
            summed = jnp.einsum('hqk,khv->qhv', probs, values)
            attn = (summed / jnp.transpose(total)[..., None]).astype(jnp.bfloat16)
            return jnp.dot(attn.reshape(block, HEADS * VDIM), out_proj, preferred_element_type=jnp.float32)
        projected = lax.map(one_block, starts).reshape(LEN, D)
        return normalize(projected, out_gain).astype(jnp.bfloat16)
    mixed = lax.map(one_sequence, tokens.reshape(SEQS, LEN, D))
    return mixed.reshape(ROWS, D)
```

```python
import functools

import jax
import jax.numpy as jnp
import numpy as np
from jax import lax
from jax.experimental import pallas as pl
from jax.experimental.pallas import tpu as pltpu
from jax.sharding import PartitionSpec as P

MESH = pl.DeviceIdType.MESH

HEADS = 4
NOPE = 128
ROPE = 64
VDIM = 128
SEQS = 8


EPS = 1e-06
THETA = 10000.0


def as_sent(value):
    return jax.tree.map(lambda a: a.astype(jnp.bfloat16) if a.dtype == jnp.float32 else a, value)


def swapped(value, axis, apart):
    mask = 2**apart
    pairs = [(source, source ^ mask) for source in range(lax.axis_size(axis))]
    return lax.ppermute(value, axis, pairs)


def normalize(rows, gain):
    mean_sq = jnp.mean(rows * rows, axis=-1, keepdims=True)
    return rows * lax.rsqrt(mean_sq + EPS) * gain


def angles(positions, width):
    half = width // 2
    freq = THETA ** (-jnp.arange(half, dtype=jnp.float32) / half)
    angle = positions[:, None] * freq[None, :]
    return (jnp.cos(angle), jnp.sin(angle))


def rotate(rows, cosine, sine):
    half = rows.shape[-1] // 2
    first = rows[..., :half]
    second = rows[..., half:]
    return jnp.concatenate(
        [first * cosine - second * sine, first * sine + second * cosine], axis=-1
    )


def join_parts(holding, incoming):
    return tuple(
        (
            jnp.concatenate([held_part, new_part], axis=0)
            for held_part, new_part in zip(holding, incoming)
        )
    )


def on_device(
    tokens,
    query_down,
    latent_down,
    rope_down,
    query_gain,
    latent_gain,
    query_up,
    query_rope,
    key_up,
    value_up,
    out_proj,
    out_gain,
):
    tp_size = lax.axis_size("tp")
    group_size = lax.axis_size("sp") // SEQS
    sections = group_size.bit_length() - 1
    heads_dev = HEADS // tp_size
    rows_dev = tokens.shape[0]
    scale = (NOPE + ROPE) ** (-0.5)
    first_row = lax.axis_index("sp") % group_size * rows_dev
    positions = (first_row + jnp.arange(rows_dev, dtype=jnp.int32)).astype(jnp.float32)
    cosine, sine = angles(positions, ROPE)
    q_latent = normalize(
        jnp.dot(tokens, query_down, preferred_element_type=jnp.float32), query_gain
    ).astype(jnp.bfloat16)
    kv_latent = normalize(
        jnp.dot(tokens, latent_down, preferred_element_type=jnp.float32), latent_gain
    ).astype(jnp.bfloat16)
    rope_key = rotate(
        jnp.dot(tokens, rope_down, preferred_element_type=jnp.float32), cosine, sine
    ).astype(jnp.bfloat16)
    q_nope = jnp.dot(q_latent, query_up, preferred_element_type=jnp.float32).astype(jnp.bfloat16)
    q_nope = q_nope.reshape(rows_dev, heads_dev, NOPE)
    q_rot = rotate(
        jnp.dot(q_latent, query_rope, preferred_element_type=jnp.float32).reshape(
            rows_dev, heads_dev, ROPE
        ),
        cosine[:, None, :],
        sine[:, None, :],
    ).astype(jnp.bfloat16)

    def expand(latent):
        keys = jnp.dot(latent, key_up, preferred_element_type=jnp.float32).astype(jnp.bfloat16)
        values = jnp.dot(latent, value_up, preferred_element_type=jnp.float32).astype(jnp.bfloat16)
        return (keys, values)

    def attend(carry, keys, values, rope_piece):
        highest, total, weighted = carry
        count = keys.shape[0]
        keys = keys.reshape(count, heads_dev, NOPE)
        values = values.reshape(count, heads_dev, VDIM)
        scores = (
            jnp.einsum("qhd,khd->hqk", q_nope, keys, preferred_element_type=jnp.float32)
            + jnp.einsum("qhr,kr->hqk", q_rot, rope_piece, preferred_element_type=jnp.float32)
        ) * scale
        new_high = jnp.maximum(highest, jnp.max(scores, axis=-1))
        factor = jnp.exp(highest - new_high)
        expd = jnp.exp(scores - new_high[..., None])
        total = total * factor + jnp.sum(expd, axis=-1)
        weighted = weighted * factor[..., None] + jnp.einsum(
            "hqk,khv->hqv", expd.astype(jnp.bfloat16), values, preferred_element_type=jnp.float32
        )
        return (new_high, total, weighted)

    carry = (
        jnp.full((heads_dev, rows_dev), -jnp.inf, jnp.float32),
        jnp.zeros((heads_dev, rows_dev), jnp.float32),
        jnp.zeros((heads_dev, rows_dev, VDIM), jnp.float32),
    )
    holding = (kv_latent, rope_key)
    own_keys, own_values = expand(kv_latent)
    carry = attend(carry, own_keys, own_values, rope_key)
    for level in range(sections):
        incoming = jax.tree.map(
            lambda part, own: part.astype(own.dtype),
            swapped(as_sent(holding), "sp", level),
            holding,
        )
        far_keys, far_values = expand(incoming[0])
        carry = attend(carry, far_keys, far_values, incoming[1])
        if level + 1 < sections:
            holding = join_parts(holding, incoming)
    highest, total, weighted = carry
    attn = (weighted / total[..., None]).astype(jnp.bfloat16)
    attn_rows = jnp.transpose(attn, (1, 0, 2)).reshape(rows_dev, heads_dev * VDIM)
    projected = jnp.dot(
        lax.all_gather(attn_rows, "tp", axis=1, tiled=True),
        out_proj,
        preferred_element_type=jnp.float32,
    )
    return normalize(projected, out_gain).astype(jnp.bfloat16)


def rotary_tables(length, width):
    half = ROPE // 2
    freq = THETA ** (-np.arange(half, dtype=np.float64) / half)
    angle = np.arange(length, dtype=np.float64)[:, None] * freq[None, :]
    cosine = np.tile(np.cos(angle), (1, width // half))
    sine = np.tile(np.concatenate([-np.sin(angle), np.sin(angle)], axis=1), (1, width // ROPE))
    return cosine.astype(np.float32), sine.astype(np.float32)


def fused_kernel(
    chunks,
    tok_h, qd_h, ld_h, rd_h, qg_h, lg_h, qu_h, qr_h, ku_h, vu_h, op_h, og_h, cos_h, sin_h,
    out_h,
    tok, qd, ld, rd, qg, lg, qu, qr, ku, vu, op, og, cosv, sinv,
    own, far, attn_own, attn_far, acc,
    in_sem, qd_sem, ld_sem, send_sem, recv_sem,
):
    rows, width = tok.shape
    latent = ku.shape[0]
    heads = ku.shape[1] // NOPE
    sp = lax.axis_index("sp")
    tp = lax.axis_index("tp")
    partner = sp + 1 - 2 * lax.rem(sp, 2)
    across = 1 - tp

    barrier = pltpu.get_barrier_semaphore()
    pl.semaphore_signal(barrier, inc=1, device_id={"sp": partner}, device_id_type=MESH)
    pl.semaphore_signal(barrier, inc=1, device_id={"tp": across}, device_id_type=MESH)

    depth = width // chunks
    mine = pl.ds(pl.multiple_of(lax.rem(sp, 2) * rows, rows), rows)
    own_rows = pl.ds(pl.multiple_of(tp * heads * VDIM, heads * VDIM), heads * VDIM)
    far_rows = pl.ds(pl.multiple_of(across * heads * VDIM, heads * VDIM), heads * VDIM)

    def copy(source, target, sem):
        made = pltpu.make_async_copy(source, target, sem)
        made.start()
        return made

    c_tok = copy(tok_h, tok, in_sem.at[0])
    c_ld = [
        copy(ld_h.at[pl.ds(k * depth, depth)], ld.at[pl.ds(k * depth, depth)], ld_sem.at[k])
        for k in range(chunks)
    ]
    c_rd = [
        copy(rd_h, rd.at[pl.ds(h * ROPE, ROPE)], in_sem.at[1 + h]) for h in range(heads)
    ]
    c_cos = copy(cos_h.at[mine], cosv, in_sem.at[3])
    c_sin = copy(sin_h.at[mine], sinv, in_sem.at[4])
    c_lg = copy(lg_h, lg, in_sem.at[5])
    c_qd = [
        copy(qd_h.at[pl.ds(k * depth, depth)], qd.at[pl.ds(k * depth, depth)], qd_sem.at[k])
        for k in range(chunks)
    ]
    c_qg = copy(qg_h, qg, in_sem.at[6])
    c_qu = copy(qu_h, qu, in_sem.at[7])
    c_qr = copy(qr_h, qr, in_sem.at[8])
    c_ku = copy(ku_h, ku, in_sem.at[9])
    c_vu = copy(vu_h, vu, in_sem.at[10])
    c_op = [
        copy(op_h.at[own_rows], op.at[0], in_sem.at[11]),
        copy(op_h.at[far_rows], op.at[1], in_sem.at[12]),
    ]
    c_og = copy(og_h, og, in_sem.at[13])

    def dot(a, b):
        return jnp.dot(a, b, preferred_element_type=jnp.float32)

    def dot_t(a, b):
        return lax.dot_general(a, b, (((1,), (1,)), ((), ())), preferred_element_type=jnp.float32)

    def down(weight, copies):
        total = None
        for k in range(chunks):
            copies[k].wait()
            part = dot(tok[:, k * depth : (k + 1) * depth], weight[k * depth : (k + 1) * depth, :])
            total = part if total is None else total + part
        return total

    lane = lax.broadcasted_iota(jnp.int32, (rows, heads * ROPE), 1)
    low = lane % ROPE < ROPE // 2

    def turned(v):
        swapped_pair = jnp.where(
            low,
            pltpu.roll(v, heads * ROPE - ROPE // 2, 1),
            pltpu.roll(v, ROPE // 2, 1),
        )
        return v * cosv[...] + swapped_pair * sinv[...]

    c_tok.wait()
    kv = down(ld, c_ld)
    c_lg.wait()
    own[:, :latent] = normalize(kv, lg[...]).astype(jnp.bfloat16)
    for c in c_rd:
        c.wait()
    c_cos.wait()
    c_sin.wait()
    own[:, latent:] = turned(dot_t(tok[...], rd[...])).astype(jnp.bfloat16)

    pl.semaphore_wait(barrier, 2)
    kv_send = pltpu.make_async_remote_copy(
        src_ref=own, dst_ref=far, send_sem=send_sem.at[0], recv_sem=recv_sem.at[0],
        device_id={"sp": partner}, device_id_type=MESH,
    )
    kv_send.start()

    q_sum = down(qd, c_qd)
    c_qg.wait()
    q_latent = normalize(q_sum, qg[...]).astype(jnp.bfloat16)
    c_qu.wait()
    q_nope = dot(q_latent, qu[...]).astype(jnp.bfloat16)
    c_qr.wait()
    q_rot = turned(dot(q_latent, qr[...])).astype(jnp.bfloat16)
    queries = [
        jnp.concatenate(
            [
                q_nope[:, h * NOPE : (h + 1) * NOPE],
                jnp.where(lane // ROPE == h, q_rot, jnp.zeros_like(q_rot)),
            ],
            axis=1,
        )
        for h in range(heads)
    ]
    c_ku.wait()
    c_vu.wait()

    def expand(block):
        latents = block[:, :latent]
        rope = block[:, latent:]
        keys = dot(latents, ku[...]).astype(jnp.bfloat16)
        values = dot(latents, vu[...]).astype(jnp.bfloat16)
        scores = [
            dot_t(queries[h], jnp.concatenate([keys[:, h * NOPE : (h + 1) * NOPE], rope], axis=1))
            for h in range(heads)
        ]
        return scores, values

    scores_own, values_own = expand(own)
    kv_send.wait_recv()
    scores_far, values_far = expand(far)
    scale = (NOPE + ROPE) ** (-0.5)
    sends = []
    for h in range(heads):
        s_own, s_far = scores_own[h], scores_far[h]
        high = jnp.maximum(
            jnp.max(s_own, axis=-1, keepdims=True), jnp.max(s_far, axis=-1, keepdims=True)
        )
        e_own = jnp.exp((s_own - high) * scale)
        e_far = jnp.exp((s_far - high) * scale)
        total = jnp.sum(e_own, axis=-1, keepdims=True) + jnp.sum(e_far, axis=-1, keepdims=True)
        cols = slice(h * VDIM, (h + 1) * VDIM)
        weighted = dot(e_own.astype(jnp.bfloat16), values_own[:, cols]) + dot(
            e_far.astype(jnp.bfloat16), values_far[:, cols]
        )
        attn_own[h] = (weighted / total).astype(jnp.bfloat16)
        send = pltpu.make_async_remote_copy(
            src_ref=attn_own.at[h], dst_ref=attn_far.at[h],
            send_sem=send_sem.at[1 + h], recv_sem=recv_sem.at[1 + h],
            device_id={"tp": across}, device_id_type=MESH,
        )
        send.start()
        sends.append(send)

    c_op[0].wait()
    held = jnp.concatenate([attn_own[h] for h in range(heads)], axis=1)
    model = op.shape[2]
    step = 512
    for n in range(0, model, step):
        acc[:, n : n + step] = dot(held, op[0, :, n : n + step])
    c_op[1].wait()
    c_og.wait()
    for send in sends:
        send.wait_recv()
    held = jnp.concatenate([attn_far[h] for h in range(heads)], axis=1)
    squares = jnp.zeros((rows, 1), jnp.float32)
    for n in range(0, model, step):
        part = acc[:, n : n + step] + dot(held, op[1, :, n : n + step])
        acc[:, n : n + step] = part
        squares = squares + jnp.sum(part * part, axis=-1, keepdims=True)
    factor = lax.rsqrt(squares / model + EPS)
    out_h[...] = (acc[...] * factor * og[...]).astype(jnp.bfloat16)
    kv_send.wait_send()
    for send in sends:
        send.wait_send()


def fused_on_device(
    tokens, query_down, latent_down, rope_down, query_gain, latent_gain,
    query_up, query_rope, key_up, value_up, out_proj, out_gain,
):
    rows, width = tokens.shape
    latent = latent_down.shape[1]
    heads = key_up.shape[1] // NOPE
    model = out_proj.shape[1]
    chunks = 4
    cosine, sine = rotary_tables(2 * rows, heads * ROPE)
    bf16, f32 = jnp.bfloat16, jnp.float32
    args = (
        tokens, query_down, latent_down, rope_down.T, query_gain[None, :], latent_gain[None, :],
        query_up, query_rope, key_up, value_up, out_proj, out_gain[None, :],
        jnp.asarray(cosine), jnp.asarray(sine),
    )
    rope_shape = (rows, heads * ROPE)
    return pl.pallas_call(
        functools.partial(fused_kernel, chunks),
        out_shape=pltpu.VMEM((rows, model), bf16),
        in_specs=[pl.BlockSpec(memory_space=pltpu.HBM)] * len(args),
        out_specs=pl.BlockSpec(memory_space=pltpu.VMEM),
        scratch_shapes=[
            pltpu.VMEM(tokens.shape, bf16),
            pltpu.VMEM(query_down.shape, bf16),
            pltpu.VMEM(latent_down.shape, bf16),
            pltpu.VMEM((heads * ROPE, width), bf16),
            pltpu.VMEM((1, latent), f32),
            pltpu.VMEM((1, latent), f32),
            pltpu.VMEM(query_up.shape, bf16),
            pltpu.VMEM(query_rope.shape, bf16),
            pltpu.VMEM(key_up.shape, bf16),
            pltpu.VMEM(value_up.shape, bf16),
            pltpu.VMEM((2, heads * VDIM, model), bf16),
            pltpu.VMEM((1, model), f32),
            pltpu.VMEM(rope_shape, f32),
            pltpu.VMEM(rope_shape, f32),
            pltpu.VMEM((rows, latent + heads * ROPE), bf16),
            pltpu.VMEM((rows, latent + heads * ROPE), bf16),
            pltpu.VMEM((heads, rows, VDIM), bf16),
            pltpu.VMEM((heads, rows, VDIM), bf16),
            pltpu.VMEM((rows, model), f32),
            pltpu.SemaphoreType.DMA((14,)),
            pltpu.SemaphoreType.DMA((chunks,)),
            pltpu.SemaphoreType.DMA((chunks,)),
            pltpu.SemaphoreType.DMA((1 + heads,)),
            pltpu.SemaphoreType.DMA((1 + heads,)),
        ],
        compiler_params=pltpu.CompilerParams(
            collective_id=0, has_side_effects=True, vmem_limit_bytes=67000000 - 2 * rows * model
        ),
    )(*args)


def solution(mesh):
    in_specs = (
        P("sp", None),
        P(),
        P(),
        P(),
        P(),
        P(),
        P(None, "tp"),
        P(None, "tp"),
        P(None, "tp"),
        P(None, "tp"),
        P(),
        P(),
    )
    out_specs = P("sp", None)
    group = mesh.shape["sp"] // SEQS
    small = group == 2 and mesh.shape["tp"] == 2 and HEADS // 2 * ROPE == 128
    return jax.shard_map(
        fused_on_device if small else on_device, mesh=mesh, in_specs=in_specs, out_specs=out_specs, check_vma=False
    )
```

```python
import functools

import jax
import jax.numpy as jnp
import numpy as np
from jax import lax
from jax.experimental import pallas as pl
from jax.experimental.pallas import tpu as pltpu
from jax.sharding import PartitionSpec as P

MESH = pl.DeviceIdType.MESH

HEADS = 4
NOPE = 128
ROPE = 64
VDIM = 128
SEQS = 8


EPS = 1e-06
THETA = 10000.0


def as_sent(value):
    return jax.tree.map(lambda a: a.astype(jnp.bfloat16) if a.dtype == jnp.float32 else a, value)


def swapped(value, axis, apart):
    mask = 2**apart
    pairs = [(source, source ^ mask) for source in range(lax.axis_size(axis))]
    return lax.ppermute(value, axis, pairs)


def normalize(rows, gain):
    mean_sq = jnp.mean(rows * rows, axis=-1, keepdims=True)
    return rows * lax.rsqrt(mean_sq + EPS) * gain


def angles(positions, width):
    half = width // 2
    freq = THETA ** (-jnp.arange(half, dtype=jnp.float32) / half)
    angle = positions[:, None] * freq[None, :]
    return (jnp.cos(angle), jnp.sin(angle))


def rotate(rows, cosine, sine):
    half = rows.shape[-1] // 2
    first = rows[..., :half]
    second = rows[..., half:]
    return jnp.concatenate(
        [first * cosine - second * sine, first * sine + second * cosine], axis=-1
    )


def join_parts(holding, incoming):
    return tuple(
        (
            jnp.concatenate([held_part, new_part], axis=0)
            for held_part, new_part in zip(holding, incoming)
        )
    )


def on_device(
    tokens,
    query_down,
    latent_down,
    rope_down,
    query_gain,
    latent_gain,
    query_up,
    query_rope,
    key_up,
    value_up,
    out_proj,
    out_gain,
):
    tp_size = lax.axis_size("tp")
    group_size = lax.axis_size("sp") // SEQS
    sections = group_size.bit_length() - 1
    heads_dev = HEADS // tp_size
    rows_dev = tokens.shape[0]
    scale = (NOPE + ROPE) ** (-0.5)
    first_row = lax.axis_index("sp") % group_size * rows_dev
    positions = (first_row + jnp.arange(rows_dev, dtype=jnp.int32)).astype(jnp.float32)
    cosine, sine = angles(positions, ROPE)
    q_latent = normalize(
        jnp.dot(tokens, query_down, preferred_element_type=jnp.float32), query_gain
    ).astype(jnp.bfloat16)
    kv_latent = normalize(
        jnp.dot(tokens, latent_down, preferred_element_type=jnp.float32), latent_gain
    ).astype(jnp.bfloat16)
    rope_key = rotate(
        jnp.dot(tokens, rope_down, preferred_element_type=jnp.float32), cosine, sine
    ).astype(jnp.bfloat16)
    q_nope = jnp.dot(q_latent, query_up, preferred_element_type=jnp.float32).astype(jnp.bfloat16)
    q_nope = q_nope.reshape(rows_dev, heads_dev, NOPE)
    q_rot = rotate(
        jnp.dot(q_latent, query_rope, preferred_element_type=jnp.float32).reshape(
            rows_dev, heads_dev, ROPE
        ),
        cosine[:, None, :],
        sine[:, None, :],
    ).astype(jnp.bfloat16)

    def expand(latent):
        keys = jnp.dot(latent, key_up, preferred_element_type=jnp.float32).astype(jnp.bfloat16)
        values = jnp.dot(latent, value_up, preferred_element_type=jnp.float32).astype(jnp.bfloat16)
        return (keys, values)

    def attend(carry, keys, values, rope_piece):
        highest, total, weighted = carry
        count = keys.shape[0]
        keys = keys.reshape(count, heads_dev, NOPE)
        values = values.reshape(count, heads_dev, VDIM)
        scores = (
            jnp.einsum("qhd,khd->hqk", q_nope, keys, preferred_element_type=jnp.float32)
            + jnp.einsum("qhr,kr->hqk", q_rot, rope_piece, preferred_element_type=jnp.float32)
        ) * scale
        new_high = jnp.maximum(highest, jnp.max(scores, axis=-1))
        factor = jnp.exp(highest - new_high)
        expd = jnp.exp(scores - new_high[..., None])
        total = total * factor + jnp.sum(expd, axis=-1)
        weighted = weighted * factor[..., None] + jnp.einsum(
            "hqk,khv->hqv", expd.astype(jnp.bfloat16), values, preferred_element_type=jnp.float32
        )
        return (new_high, total, weighted)

    carry = (
        jnp.full((heads_dev, rows_dev), -jnp.inf, jnp.float32),
        jnp.zeros((heads_dev, rows_dev), jnp.float32),
        jnp.zeros((heads_dev, rows_dev, VDIM), jnp.float32),
    )
    holding = (kv_latent, rope_key)
    own_keys, own_values = expand(kv_latent)
    carry = attend(carry, own_keys, own_values, rope_key)
    for level in range(sections):
        incoming = jax.tree.map(
            lambda part, own: part.astype(own.dtype),
            swapped(as_sent(holding), "sp", level),
            holding,
        )
        far_keys, far_values = expand(incoming[0])
        carry = attend(carry, far_keys, far_values, incoming[1])
        if level + 1 < sections:
            holding = join_parts(holding, incoming)
    highest, total, weighted = carry
    attn = (weighted / total[..., None]).astype(jnp.bfloat16)
    attn_rows = jnp.transpose(attn, (1, 0, 2)).reshape(rows_dev, heads_dev * VDIM)
    projected = jnp.dot(
        lax.all_gather(attn_rows, "tp", axis=1, tiled=True),
        out_proj,
        preferred_element_type=jnp.float32,
    )
    return normalize(projected, out_gain).astype(jnp.bfloat16)


def rotary_tables(length, width):
    half = ROPE // 2
    freq = THETA ** (-np.arange(half, dtype=np.float64) / half)
    angle = np.arange(length, dtype=np.float64)[:, None] * freq[None, :]
    cosine = np.tile(np.cos(angle), (1, width // half))
    sine = np.tile(np.concatenate([-np.sin(angle), np.sin(angle)], axis=1), (1, width // ROPE))
    return cosine.astype(np.float32), sine.astype(np.float32)


def fused_kernel(
    chunks,
    tok_h, qd_h, ld_h, rd_h, qg_h, lg_h, qu_h, qr_h, ku_h, vu_h, op_h, og_h, cos_h, sin_h,
    out_h,
    tok, qd, ld, rd, qg, lg, qu, qr, ku, vu, op, og, cosv, sinv,
    own, far, attn_own, attn_far, acc,
    in_sem, qd_sem, ld_sem, send_sem, recv_sem,
):
    rows, width = tok.shape
    latent = ku.shape[0]
    heads = ku.shape[1] // NOPE
    sp = lax.axis_index("sp")
    tp = lax.axis_index("tp")
    partner = sp + 1 - 2 * lax.rem(sp, 2)
    across = 1 - tp

    barrier = pltpu.get_barrier_semaphore()
    pl.semaphore_signal(barrier, inc=1, device_id={"sp": partner}, device_id_type=MESH)
    pl.semaphore_signal(barrier, inc=1, device_id={"tp": across}, device_id_type=MESH)

    depth = width // chunks
    mine = pl.ds(pl.multiple_of(lax.rem(sp, 2) * rows, rows), rows)
    own_rows = pl.ds(pl.multiple_of(tp * heads * VDIM, heads * VDIM), heads * VDIM)
    far_rows = pl.ds(pl.multiple_of(across * heads * VDIM, heads * VDIM), heads * VDIM)

    def copy(source, target, sem):
        made = pltpu.make_async_copy(source, target, sem)
        made.start()
        return made

    def pieces(source, target, sem):
        return [
            copy(source.at[pl.ds(k * depth, depth)], target.at[pl.ds(k * depth, depth)], sem.at[k])
            for k in range(chunks)
        ]

    c_tok = copy(tok_h, tok, in_sem.at[0])
    c_rd = copy(rd_h, rd, in_sem.at[1])
    c_latent = pieces(ld_h, ld, ld_sem) + [
        copy(lg_h, lg, in_sem.at[4]),
        copy(cos_h.at[mine], cosv, in_sem.at[2]),
        copy(sin_h.at[mine], sinv, in_sem.at[3]),
    ]

    def dot(a, b):
        return jnp.dot(a, b, preferred_element_type=jnp.float32)

    def dot_t(a, b):
        return lax.dot_general(a, b, (((1,), (1,)), ((), ())), preferred_element_type=jnp.float32)

    lane = lax.broadcasted_iota(jnp.int32, (rows, heads * ROPE), 1)
    low = lane % ROPE < ROPE // 2

    def turned(v):
        swapped_pair = jnp.where(
            low,
            pltpu.roll(v, heads * ROPE - ROPE // 2, 1),
            pltpu.roll(v, ROPE // 2, 1),
        )
        return v * cosv[...] + swapped_pair * sinv[...]

    pl.delay(150)
    c_expand = [copy(ku_h, ku, in_sem.at[8]), copy(vu_h, vu, in_sem.at[9])]
    c_query = pieces(qd_h, qd, qd_sem) + [
        copy(qg_h, qg, in_sem.at[5]),
        copy(qu_h, qu, in_sem.at[6]),
        copy(qr_h, qr, in_sem.at[7]),
    ]
    c_tok.wait()
    c_rd.wait()
    rope_raw = dot_t(tok[...], jnp.concatenate([rd[...]] * heads, axis=0))
    for c in c_latent:
        c.wait()
    kv = dot(tok[...], ld[...])
    own[:, latent:] = turned(rope_raw).astype(jnp.bfloat16)
    own[:, :latent] = normalize(kv, lg[...]).astype(jnp.bfloat16)
    pl.semaphore_wait(barrier, 2)
    kv_send = pltpu.make_async_remote_copy(
        src_ref=own, dst_ref=far, send_sem=send_sem.at[0], recv_sem=recv_sem.at[0],
        device_id={"sp": partner}, device_id_type=MESH,
    )
    kv_send.start()

    def expand(block):
        latents = block[:, :latent]
        keys = dot(latents, ku[...]).astype(jnp.bfloat16)
        values = dot(latents, vu[...]).astype(jnp.bfloat16)
        return keys, block[:, latent:], values

    c_out = [
        copy(op_h.at[own_rows], op.at[0], in_sem.at[10]),
        copy(op_h.at[far_rows], op.at[1], in_sem.at[11]),
        copy(og_h, og, in_sem.at[12]),
    ]
    for c in c_expand:
        c.wait()
    held_own = expand(own)
    for c in c_query:
        c.wait()
    q_raw = dot(tok[...], qd[...])
    q_factor = lax.rsqrt(jnp.mean(q_raw * q_raw, axis=-1, keepdims=True) + EPS)
    q_gained = (q_raw * qg[...]).astype(jnp.bfloat16)
    q_nope = (dot(q_gained, qu[...]) * q_factor).astype(jnp.bfloat16)
    q_rot = (turned(dot(q_gained, qr[...])) * q_factor).astype(jnp.bfloat16)
    queries = [
        jnp.concatenate(
            [
                q_nope[:, h * NOPE : (h + 1) * NOPE],
                jnp.where(lane // ROPE == h, q_rot, jnp.zeros_like(q_rot)),
            ],
            axis=1,
        )
        for h in range(heads)
    ]
    def score(held, h):
        keys, rope, _ = held
        full = jnp.concatenate([keys[:, h * NOPE : (h + 1) * NOPE], rope], axis=1)
        return dot_t(queries[h], full)

    kv_send.wait_recv()
    held_far = expand(far)
    scores_own = [score(held_own, h) for h in range(heads)]
    scale = (NOPE + ROPE) ** (-0.5)
    sends = []
    for h in range(heads):
        s_own, s_far = scores_own[h], score(held_far, h)
        high = jnp.maximum(
            jnp.max(s_own, axis=-1, keepdims=True), jnp.max(s_far, axis=-1, keepdims=True)
        )
        e_own = jnp.exp((s_own - high) * scale)
        e_far = jnp.exp((s_far - high) * scale)
        total = jnp.sum(e_own, axis=-1, keepdims=True) + jnp.sum(e_far, axis=-1, keepdims=True)
        cols = slice(h * VDIM, (h + 1) * VDIM)
        weighted = dot(e_own.astype(jnp.bfloat16), held_own[2][:, cols]) + dot(
            e_far.astype(jnp.bfloat16), held_far[2][:, cols]
        )
        attn_own[h] = (weighted / total).astype(jnp.bfloat16)
        send = pltpu.make_async_remote_copy(
            src_ref=attn_own.at[h], dst_ref=attn_far.at[h],
            send_sem=send_sem.at[1 + h], recv_sem=recv_sem.at[1 + h],
            device_id={"tp": across}, device_id_type=MESH,
        )
        send.start()
        sends.append(send)

    for c in c_out:
        c.wait()
    held = jnp.concatenate([attn_own[h] for h in range(heads)], axis=1)
    model = op.shape[2]
    step = 512
    for n in range(0, model, step):
        acc[:, n : n + step] = dot(held, op[0, :, n : n + step])
    for send in sends:
        send.wait_recv()
    held = jnp.concatenate([attn_far[h] for h in range(heads)], axis=1)
    squares = jnp.zeros((rows, 1), jnp.float32)
    for n in range(0, model, step):
        part = acc[:, n : n + step] + dot(held, op[1, :, n : n + step])
        acc[:, n : n + step] = part
        squares = squares + jnp.sum(part * part, axis=-1, keepdims=True)
    factor = lax.rsqrt(squares / model + EPS)
    out_h[...] = (acc[...] * factor * og[...]).astype(jnp.bfloat16)
    kv_send.wait_send()
    for send in sends:
        send.wait_send()


def fused_on_device(
    tokens, query_down, latent_down, rope_down, query_gain, latent_gain,
    query_up, query_rope, key_up, value_up, out_proj, out_gain,
):
    rows, width = tokens.shape
    latent = latent_down.shape[1]
    heads = key_up.shape[1] // NOPE
    model = out_proj.shape[1]
    chunks = 4
    cosine, sine = rotary_tables(2 * rows, heads * ROPE)
    bf16, f32 = jnp.bfloat16, jnp.float32
    args = (
        tokens, query_down, latent_down, rope_down.T, query_gain[None, :], latent_gain[None, :],
        query_up, query_rope, key_up, value_up, out_proj, out_gain[None, :],
        jnp.asarray(cosine), jnp.asarray(sine),
    )
    rope_shape = (rows, heads * ROPE)
    return pl.pallas_call(
        functools.partial(fused_kernel, chunks),
        out_shape=pltpu.VMEM((rows, model), bf16),
        in_specs=[pl.BlockSpec(memory_space=pltpu.HBM)] * len(args),
        out_specs=pl.BlockSpec(memory_space=pltpu.VMEM),
        scratch_shapes=[
            pltpu.VMEM(tokens.shape, bf16),
            pltpu.VMEM(query_down.shape, bf16),
            pltpu.VMEM(latent_down.shape, bf16),
            pltpu.VMEM((ROPE, width), bf16),
            pltpu.VMEM((1, latent), f32),
            pltpu.VMEM((1, latent), f32),
            pltpu.VMEM(query_up.shape, bf16),
            pltpu.VMEM(query_rope.shape, bf16),
            pltpu.VMEM(key_up.shape, bf16),
            pltpu.VMEM(value_up.shape, bf16),
            pltpu.VMEM((2, heads * VDIM, model), bf16),
            pltpu.VMEM((1, model), f32),
            pltpu.VMEM(rope_shape, f32),
            pltpu.VMEM(rope_shape, f32),
            pltpu.VMEM((rows, latent + heads * ROPE), bf16),
            pltpu.VMEM((rows, latent + heads * ROPE), bf16),
            pltpu.VMEM((heads, rows, VDIM), bf16),
            pltpu.VMEM((heads, rows, VDIM), bf16),
            pltpu.VMEM((rows, model), f32),
            pltpu.SemaphoreType.DMA((14,)),
            pltpu.SemaphoreType.DMA((chunks,)),
            pltpu.SemaphoreType.DMA((chunks,)),
            pltpu.SemaphoreType.DMA((1 + heads,)),
            pltpu.SemaphoreType.DMA((1 + heads,)),
        ],
        compiler_params=pltpu.CompilerParams(
            collective_id=0, has_side_effects=True, vmem_limit_bytes=67000000 - 2 * rows * model
        ),
    )(*args)


def solution(mesh):
    in_specs = (
        P("sp", None),
        P(),
        P(),
        P(),
        P(),
        P(),
        P(None, "tp"),
        P(None, "tp"),
        P(None, "tp"),
        P(None, "tp"),
        P(),
        P(),
    )
    out_specs = P("sp", None)
    group = mesh.shape["sp"] // SEQS
    small = group == 2 and mesh.shape["tp"] == 2 and HEADS // 2 * ROPE == 128
    return jax.shard_map(
        fused_on_device if small else on_device, mesh=mesh, in_specs=in_specs, out_specs=out_specs, check_vma=False
    )
```

```python
import functools

import jax
import jax.numpy as jnp
import numpy as np
from jax import lax
from jax.experimental import pallas as pl
from jax.experimental.pallas import tpu as pltpu
from jax.sharding import PartitionSpec as P

MESH = pl.DeviceIdType.MESH

HEADS = 4
NOPE = 128
ROPE = 64
VDIM = 128
SEQS = 8


EPS = 1e-06
THETA = 10000.0


def as_sent(value):
    return jax.tree.map(lambda a: a.astype(jnp.bfloat16) if a.dtype == jnp.float32 else a, value)


def swapped(value, axis, apart):
    mask = 2**apart
    pairs = [(source, source ^ mask) for source in range(lax.axis_size(axis))]
    return lax.ppermute(value, axis, pairs)


def normalize(rows, gain):
    mean_sq = jnp.mean(rows * rows, axis=-1, keepdims=True)
    return rows * lax.rsqrt(mean_sq + EPS) * gain


def angles(positions, width):
    half = width // 2
    freq = THETA ** (-jnp.arange(half, dtype=jnp.float32) / half)
    angle = positions[:, None] * freq[None, :]
    return (jnp.cos(angle), jnp.sin(angle))


def rotate(rows, cosine, sine):
    half = rows.shape[-1] // 2
    first = rows[..., :half]
    second = rows[..., half:]
    return jnp.concatenate(
        [first * cosine - second * sine, first * sine + second * cosine], axis=-1
    )


def join_parts(holding, incoming):
    return tuple(
        (
            jnp.concatenate([held_part, new_part], axis=0)
            for held_part, new_part in zip(holding, incoming)
        )
    )


def on_device(
    tokens,
    query_down,
    latent_down,
    rope_down,
    query_gain,
    latent_gain,
    query_up,
    query_rope,
    key_up,
    value_up,
    out_proj,
    out_gain,
):
    tp_size = lax.axis_size("tp")
    group_size = lax.axis_size("sp") // SEQS
    sections = group_size.bit_length() - 1
    heads_dev = HEADS // tp_size
    rows_dev = tokens.shape[0]
    scale = (NOPE + ROPE) ** (-0.5)
    first_row = lax.axis_index("sp") % group_size * rows_dev
    positions = (first_row + jnp.arange(rows_dev, dtype=jnp.int32)).astype(jnp.float32)
    cosine, sine = angles(positions, ROPE)
    q_latent = normalize(
        jnp.dot(tokens, query_down, preferred_element_type=jnp.float32), query_gain
    ).astype(jnp.bfloat16)
    kv_latent = normalize(
        jnp.dot(tokens, latent_down, preferred_element_type=jnp.float32), latent_gain
    ).astype(jnp.bfloat16)
    rope_key = rotate(
        jnp.dot(tokens, rope_down, preferred_element_type=jnp.float32), cosine, sine
    ).astype(jnp.bfloat16)
    q_nope = jnp.dot(q_latent, query_up, preferred_element_type=jnp.float32).astype(jnp.bfloat16)
    q_nope = q_nope.reshape(rows_dev, heads_dev, NOPE)
    q_rot = rotate(
        jnp.dot(q_latent, query_rope, preferred_element_type=jnp.float32).reshape(
            rows_dev, heads_dev, ROPE
        ),
        cosine[:, None, :],
        sine[:, None, :],
    ).astype(jnp.bfloat16)

    def expand(latent):
        keys = jnp.dot(latent, key_up, preferred_element_type=jnp.float32).astype(jnp.bfloat16)
        values = jnp.dot(latent, value_up, preferred_element_type=jnp.float32).astype(jnp.bfloat16)
        return (keys, values)

    def attend(carry, keys, values, rope_piece):
        highest, total, weighted = carry
        count = keys.shape[0]
        keys = keys.reshape(count, heads_dev, NOPE)
        values = values.reshape(count, heads_dev, VDIM)
        scores = (
            jnp.einsum("qhd,khd->hqk", q_nope, keys, preferred_element_type=jnp.float32)
            + jnp.einsum("qhr,kr->hqk", q_rot, rope_piece, preferred_element_type=jnp.float32)
        ) * scale
        new_high = jnp.maximum(highest, jnp.max(scores, axis=-1))
        factor = jnp.exp(highest - new_high)
        expd = jnp.exp(scores - new_high[..., None])
        total = total * factor + jnp.sum(expd, axis=-1)
        weighted = weighted * factor[..., None] + jnp.einsum(
            "hqk,khv->hqv", expd.astype(jnp.bfloat16), values, preferred_element_type=jnp.float32
        )
        return (new_high, total, weighted)

    carry = (
        jnp.full((heads_dev, rows_dev), -jnp.inf, jnp.float32),
        jnp.zeros((heads_dev, rows_dev), jnp.float32),
        jnp.zeros((heads_dev, rows_dev, VDIM), jnp.float32),
    )
    holding = (kv_latent, rope_key)
    own_keys, own_values = expand(kv_latent)
    carry = attend(carry, own_keys, own_values, rope_key)
    for level in range(sections):
        incoming = jax.tree.map(
            lambda part, own: part.astype(own.dtype),
            swapped(as_sent(holding), "sp", level),
            holding,
        )
        far_keys, far_values = expand(incoming[0])
        carry = attend(carry, far_keys, far_values, incoming[1])
        if level + 1 < sections:
            holding = join_parts(holding, incoming)
    highest, total, weighted = carry
    attn = (weighted / total[..., None]).astype(jnp.bfloat16)
    attn_rows = jnp.transpose(attn, (1, 0, 2)).reshape(rows_dev, heads_dev * VDIM)
    projected = jnp.dot(
        lax.all_gather(attn_rows, "tp", axis=1, tiled=True),
        out_proj,
        preferred_element_type=jnp.float32,
    )
    return normalize(projected, out_gain).astype(jnp.bfloat16)


def rotary_tables(length, width):
    half = ROPE // 2
    freq = THETA ** (-np.arange(half, dtype=np.float64) / half)
    angle = np.arange(length, dtype=np.float64)[:, None] * freq[None, :]
    cosine = np.tile(np.cos(angle), (1, width // half))
    sine = np.tile(np.concatenate([-np.sin(angle), np.sin(angle)], axis=1), (1, width // ROPE))
    return cosine.astype(np.float32), sine.astype(np.float32)


def fused_kernel(
    chunks,
    tok_h, qd_h, ld_h, rd_h, qg_h, lg_h, qu_h, qr_h, ku_h, vu_h, op_h, og_h, cos_h, sin_h,
    out_h,
    tok, qd, ld, rd, qg, lg, qu, qr, ku, vu, op, og, cosv, sinv,
    own, far, attn_own, attn_far, acc,
    in_sem, qd_sem, ld_sem, send_sem, recv_sem,
):
    rows, width = tok.shape
    latent = ku.shape[0]
    heads = ku.shape[1] // NOPE
    sp = lax.axis_index("sp")
    tp = lax.axis_index("tp")
    partner = sp + 1 - 2 * lax.rem(sp, 2)
    across = 1 - tp

    barrier = pltpu.get_barrier_semaphore()
    pl.semaphore_signal(barrier, inc=1, device_id={"sp": partner}, device_id_type=MESH)
    pl.semaphore_signal(barrier, inc=1, device_id={"tp": across}, device_id_type=MESH)

    depth = width // chunks
    mine = pl.ds(pl.multiple_of(lax.rem(sp, 2) * rows, rows), rows)
    own_rows = pl.ds(pl.multiple_of(tp * heads * VDIM, heads * VDIM), heads * VDIM)
    far_rows = pl.ds(pl.multiple_of(across * heads * VDIM, heads * VDIM), heads * VDIM)

    def copy(source, target, sem):
        made = pltpu.make_async_copy(source, target, sem)
        made.start()
        return made

    def pieces(source, target, sem):
        return [
            copy(source.at[pl.ds(k * depth, depth)], target.at[pl.ds(k * depth, depth)], sem.at[k])
            for k in range(chunks)
        ]

    c_tok = copy(tok_h, tok, in_sem.at[0])
    c_rd = copy(rd_h, rd, in_sem.at[1])
    c_latent = pieces(ld_h, ld, ld_sem) + [
        copy(lg_h, lg, in_sem.at[4]),
        copy(cos_h.at[mine], cosv, in_sem.at[2]),
        copy(sin_h.at[mine], sinv, in_sem.at[3]),
    ]

    def dot(a, b):
        return jnp.dot(a, b, preferred_element_type=jnp.float32)

    def dot_t(a, b):
        return lax.dot_general(a, b, (((1,), (1,)), ((), ())), preferred_element_type=jnp.float32)

    lane = lax.broadcasted_iota(jnp.int32, (rows, heads * ROPE), 1)
    low = lane % ROPE < ROPE // 2

    def turned(v):
        swapped_pair = jnp.where(
            low,
            pltpu.roll(v, heads * ROPE - ROPE // 2, 1),
            pltpu.roll(v, ROPE // 2, 1),
        )
        return v * cosv[...] + swapped_pair * sinv[...]

    pl.delay(150)
    c_expand = [copy(ku_h, ku, in_sem.at[8]), copy(vu_h, vu, in_sem.at[9])]
    c_query = pieces(qd_h, qd, qd_sem) + [
        copy(qg_h, qg, in_sem.at[5]),
        copy(qu_h, qu, in_sem.at[6]),
        copy(qr_h, qr, in_sem.at[7]),
    ]
    c_tok.wait()
    c_rd.wait()
    rope_raw = dot_t(tok[...], jnp.concatenate([rd[...]] * heads, axis=0))
    for c in c_latent:
        c.wait()
    kv = dot(tok[...], ld[...])
    own[:, latent:] = turned(rope_raw).astype(jnp.bfloat16)
    own[:, :latent] = normalize(kv, lg[...]).astype(jnp.bfloat16)
    pl.semaphore_wait(barrier, 2)
    kv_send = pltpu.make_async_remote_copy(
        src_ref=own, dst_ref=far, send_sem=send_sem.at[0], recv_sem=recv_sem.at[0],
        device_id={"sp": partner}, device_id_type=MESH,
    )
    kv_send.start()

    def expand(block):
        latents = block[:, :latent]
        keys = dot(latents, ku[...]).astype(jnp.bfloat16)
        values = dot(latents, vu[...]).astype(jnp.bfloat16)
        return keys, block[:, latent:], values

    c_out = [
        copy(op_h.at[own_rows], op.at[0], in_sem.at[10]),
        copy(op_h.at[far_rows], op.at[1], in_sem.at[11]),
        copy(og_h, og, in_sem.at[12]),
    ]
    for c in c_expand:
        c.wait()
    held_own = expand(own)
    for c in c_query:
        c.wait()
    q_raw = dot(tok[...], qd[...])
    q_factor = lax.rsqrt(jnp.mean(q_raw * q_raw, axis=-1, keepdims=True) + EPS)
    q_gained = (q_raw * qg[...]).astype(jnp.bfloat16)
    q_nope = (dot(q_gained, qu[...]) * q_factor).astype(jnp.bfloat16)
    q_rot = (turned(dot(q_gained, qr[...])) * q_factor).astype(jnp.bfloat16)
    queries = [
        jnp.concatenate(
            [
                q_nope[:, h * NOPE : (h + 1) * NOPE],
                jnp.where(lane // ROPE == h, q_rot, jnp.zeros_like(q_rot)),
            ],
            axis=1,
        )
        for h in range(heads)
    ]
    def score(held, h):
        keys, rope, _ = held
        full = jnp.concatenate([keys[:, h * NOPE : (h + 1) * NOPE], rope], axis=1)
        return dot_t(queries[h], full)

    kv_send.wait_recv()
    held_far = expand(far)
    scores_own = [score(held_own, h) for h in range(heads)]
    scale = (NOPE + ROPE) ** (-0.5)
    sends = []
    for h in range(heads):
        s_own, s_far = scores_own[h], score(held_far, h)
        high = jnp.max(jnp.maximum(s_own, s_far), axis=-1, keepdims=True)
        e_own = jnp.exp((s_own - high) * scale)
        e_far = jnp.exp((s_far - high) * scale)
        total = jnp.sum(e_own + e_far, axis=-1, keepdims=True)
        cols = slice(h * VDIM, (h + 1) * VDIM)
        weighted = dot(e_own.astype(jnp.bfloat16), held_own[2][:, cols]) + dot(
            e_far.astype(jnp.bfloat16), held_far[2][:, cols]
        )
        attn_own[h] = (weighted / total).astype(jnp.bfloat16)
        send = pltpu.make_async_remote_copy(
            src_ref=attn_own.at[h], dst_ref=attn_far.at[h],
            send_sem=send_sem.at[1 + h], recv_sem=recv_sem.at[1 + h],
            device_id={"tp": across}, device_id_type=MESH,
        )
        send.start()
        sends.append(send)

    for c in c_out:
        c.wait()
    held = jnp.concatenate([attn_own[h] for h in range(heads)], axis=1)
    model = op.shape[2]
    step = 512
    for n in range(0, model, step):
        acc[:, n : n + step] = dot(held, op[0, :, n : n + step])
    for send in sends:
        send.wait_recv()
    held = jnp.concatenate([attn_far[h] for h in range(heads)], axis=1)
    squares = jnp.zeros((rows, 1), jnp.float32)
    for n in range(0, model, step):
        part = acc[:, n : n + step] + dot(held, op[1, :, n : n + step])
        acc[:, n : n + step] = part
        squares = squares + jnp.sum(part * part, axis=-1, keepdims=True)
    factor = lax.rsqrt(squares / model + EPS)
    out_h[...] = (acc[...] * factor * og[...]).astype(jnp.bfloat16)
    kv_send.wait_send()
    for send in sends:
        send.wait_send()


def fused_on_device(
    tokens, query_down, latent_down, rope_down, query_gain, latent_gain,
    query_up, query_rope, key_up, value_up, out_proj, out_gain,
):
    rows, width = tokens.shape
    latent = latent_down.shape[1]
    heads = key_up.shape[1] // NOPE
    model = out_proj.shape[1]
    chunks = 4
    cosine, sine = rotary_tables(2 * rows, heads * ROPE)
    bf16, f32 = jnp.bfloat16, jnp.float32
    args = (
        tokens, query_down, latent_down, rope_down.T, query_gain[None, :], latent_gain[None, :],
        query_up, query_rope, key_up, value_up, out_proj, out_gain[None, :],
        jnp.asarray(cosine), jnp.asarray(sine),
    )
    rope_shape = (rows, heads * ROPE)
    return pl.pallas_call(
        functools.partial(fused_kernel, chunks),
        out_shape=pltpu.VMEM((rows, model), bf16),
        in_specs=[pl.BlockSpec(memory_space=pltpu.HBM)] * len(args),
        out_specs=pl.BlockSpec(memory_space=pltpu.VMEM),
        scratch_shapes=[
            pltpu.VMEM(tokens.shape, bf16),
            pltpu.VMEM(query_down.shape, bf16),
            pltpu.VMEM(latent_down.shape, bf16),
            pltpu.VMEM((ROPE, width), bf16),
            pltpu.VMEM((1, latent), f32),
            pltpu.VMEM((1, latent), f32),
            pltpu.VMEM(query_up.shape, bf16),
            pltpu.VMEM(query_rope.shape, bf16),
            pltpu.VMEM(key_up.shape, bf16),
            pltpu.VMEM(value_up.shape, bf16),
            pltpu.VMEM((2, heads * VDIM, model), bf16),
            pltpu.VMEM((1, model), f32),
            pltpu.VMEM(rope_shape, f32),
            pltpu.VMEM(rope_shape, f32),
            pltpu.VMEM((rows, latent + heads * ROPE), bf16),
            pltpu.VMEM((rows, latent + heads * ROPE), bf16),
            pltpu.VMEM((heads, rows, VDIM), bf16),
            pltpu.VMEM((heads, rows, VDIM), bf16),
            pltpu.VMEM((rows, model), f32),
            pltpu.SemaphoreType.DMA((14,)),
            pltpu.SemaphoreType.DMA((chunks,)),
            pltpu.SemaphoreType.DMA((chunks,)),
            pltpu.SemaphoreType.DMA((1 + heads,)),
            pltpu.SemaphoreType.DMA((1 + heads,)),
        ],
        compiler_params=pltpu.CompilerParams(
            collective_id=0, has_side_effects=True, vmem_limit_bytes=67000000 - 2 * rows * model
        ),
    )(*args)


def solution(mesh):
    in_specs = (
        P("sp", None),
        P(),
        P(),
        P(),
        P(),
        P(),
        P(None, "tp"),
        P(None, "tp"),
        P(None, "tp"),
        P(None, "tp"),
        P(),
        P(),
    )
    out_specs = P("sp", None)
    group = mesh.shape["sp"] // SEQS
    small = group == 2 and mesh.shape["tp"] == 2 and HEADS // 2 * ROPE == 128
    return jax.shard_map(
        fused_on_device if small else on_device, mesh=mesh, in_specs=in_specs, out_specs=out_specs, check_vma=False
    )
```
